32 devices in a mesh: sp: 8 (over z, x), tp: 4 (over y, core).
Axes of the slice: x: 2, y: 2, z: 4, core: 2. Of those that a mesh axis runs over, the one named last changes fastest.
Arguments:
- glu_a: bfloat16 [2048, 1024], P('sp', 'tp'), may hold values from -6 to 6
- glu_b: bfloat16 [2048, 1024], P('sp', 'tp'), may hold values from -6 to 6
- saved_conv: bfloat16 [2048, 1024], P('sp', 'tp')
- taps: float32 [31, 1024], P(None, 'tp'), may hold values from -1 to 1
- norm_gain_vector: float32 [1024], P('tp'), may hold values from 0.1 to 1.9
- out_proj: bfloat16 [1024, 2048], P('tp'), may hold values from -0.1875 to 0.1875
- moe_in: bfloat16 [2048, 2048], P('sp'), may hold values from -6 to 6
- grad_out: bfloat16 [2048, 2048], P('sp'), may hold values from -6 to 6
- expert_ids: int32 [2048, 2], P('sp'), may hold values from 0 to 7, all different within a row; in each aligned block of 256 rows (0 to 255, 256 to 511, ...) at most 96 rows name the same one
- route_weights: float32 [2048, 2], P('sp'), may hold values from 0.3 to 2
- w_gate: bfloat16 [8, 2048, 1024], P('sp', None, 'tp'), may hold values from -0.125 to 0.125
- w_up: bfloat16 [8, 2048, 1024], P('sp', None, 'tp'), may hold values from -0.125 to 0.125
- w_down: bfloat16 [8, 1024, 2048], P('sp', 'tp'), may hold values from -0.1875 to 0.1875
Outputs:
- grad_glu_a: bfloat16 [2048, 1024], P('sp', 'tp')
- grad_glu_b: bfloat16 [2048, 1024], P('sp', 'tp')
- grad_out_proj: float32 [2048, 1024], P('sp', 'tp')
- grad_gate: bfloat16 [8, 2048, 1024], P('sp', None, 'tp')
- grad_up: bfloat16 [8, 2048, 1024], P('sp', None, 'tp')
- grad_down: bfloat16 [8, 1024, 2048], P('sp', 'tp')
The draws below stay inside these ranges and needn't reach their ends.
Inputs may be any that keep to these rules, and one draw needn't show every extreme that they name: `expert_ids`: in each aligned block of 256 tokens, a token's 2 experts differ, and no expert is named more than 96 times; some expert reaches 96 in some blocks.
All inputs are finite; a program needn't handle non-finite values.
Results may differ from the reference program's by a relative error of at most 0.015.
Values may be sent and summed in bfloat16 or wider, within the bound.
A program may use at most 64 MiB of HBM per device.

```python
import math
import jax
import jax.numpy as jnp
import numpy as np
from jax import lax

D = 2048
CONV_CHANNELS = 1024
FF = 1024
KW = 31
TOPK = 2
TOK_DEV = 256
TOKENS = 2048
EXPERTS = 8
CAP = 96
N_SP = 8
N_TP = 4


def draw_saved_conv(key, part):
    key_base = jax.random.fold_in(key, 11)
    key_row = jax.random.fold_in(key, 12)
    key_chan = jax.random.fold_in(key, 13)
    base = jax.random.normal(key_base, (TOKENS, CONV_CHANNELS), jnp.float32)
    rising = jnp.exp(jnp.log(4.0) * jnp.arange(CONV_CHANNELS, dtype=jnp.float32) / CONV_CHANNELS)
    rough = jax.random.uniform(key_chan, (CONV_CHANNELS,), jnp.float32, 0.5, 1.5)
    row_scale = jax.random.uniform(key_row, (TOKENS, 1), jnp.float32, 0.6, 1.6)
    values = base * rising[None, :] * rough[None, :] * row_scale * 0.5
    return values.astype(jnp.bfloat16)


def raised(array, key, source, target, shards_of, factor):
    owner, partner = [(jnp.arange(array.shape[axis_at]) // (array.shape[axis_at] // shards_of)).reshape([-1 if axis == axis_at else 1 for axis in range(array.ndim)]) for axis_at in (source, target)]
    chosen = jax.random.permutation(key, shards_of)[partner]
    strong = (owner == chosen) | (owner == (partner + shards_of // 2) % shards_of)
    return jnp.where(strong, factor * array, array)


def block_scale(stream_key, shape, split, least, top_value):
    def one(dim, parts):
        heights = jax.random.uniform(jax.random.fold_in(jax.random.fold_in(stream_key, 6), dim), (parts,), jnp.float32, least / len(split), top_value / len(split))
        return jnp.repeat(jnp.exp(heights), shape[dim] // parts).reshape((-1,) + (1,) * (len(shape) - dim - 1))

    loudness = one(*split[0])
    for cut in split[1:]:
        loudness = loudness * one(*cut)
    return loudness


def deal_out(key, own, number, rows, number_of, top, limit, lean):
    order = jax.random.permutation(key, number_of)
    packed, usual = shares(number_of, rows * top, limit, lean, True), shares(number_of, rows * top, limit, lean, False)
    places = jnp.arange(number_of)

    def named(lengths, rotation):
        used = int((lengths > 0).sum())
        fixed = max(1, used // 4)
        moved = fixed + (places - fixed + rotation * (used - fixed)) % max(1, number_of - fixed)
        return jnp.zeros((number_of,), jnp.int32).at[order[jnp.where(places < fixed, places, moved)]].set(jnp.asarray(lengths, jnp.int32))

    lengths = jnp.where(number % 4 == 0, named(packed, number // 4), named(usual, number - number // 4 - 1))
    mixed = jax.random.permutation(jax.random.fold_in(own, 3), number_of)
    source_of, receiver = mixed[0:number_of // 2 * 2:2], mixed[1:number_of // 2 * 2:2]
    room = jnp.minimum(lengths[source_of] - 1, limit - lengths[receiver]) // 2
    room = jnp.where((source_of == order[0]) | (receiver == order[0]) | (lengths[receiver] == 0), 0, jnp.maximum(room, 0))
    moved = jax.random.randint(jax.random.fold_in(own, 4), (number_of // 2,), 0, 1 << 20) % (room + 1)
    lengths = lengths.at[source_of].add(-moved).at[receiver].add(moved)
    items = jnp.searchsorted(jnp.cumsum(lengths), jnp.arange(rows * top), side="right").astype(jnp.int32)
    table = items.reshape(top, rows).T
    table = table[jax.random.permutation(jax.random.fold_in(own, 1), rows)]
    rotation = jax.random.randint(jax.random.fold_in(own, 2), (rows, 1), 0, top)
    return jnp.take_along_axis(table, (jnp.arange(top)[None, :] + rotation) % top, axis=1)


def shares(count, total, limit, lean, full):
    weights = [(1 << 20) // math.isqrt(grade ** lean) + 1 for grade in range(1, count + 1)]
    largest = limit if full else min(limit, max(-(-total // count), total * weights[0] // sum(weights)))
    least = 1 if total - largest >= count - 1 else 0
    given, surplus = [largest] + [least] * (count - 1), total - largest - least * (count - 1)
    while surplus > 0:
        free = [i for i in range(1, count) if given[i] < largest] or [i for i in range(1, count) if given[i] < limit]
        whole, remaining = sum([weights[i] for i in free]), surplus
        for i in free:
            more = min(limit - given[i], max(1, remaining * weights[i] // whole), surplus)
            given[i] = given[i] + more
            surplus = surplus - more
    return np.array(given)


def normal_values(rng, shape, deviation, most, shards=(), held_as=jnp.bfloat16):
    factor_of = block_scale(rng, shape, shards, -0.22, 0.18) if shards else 1.0
    drawn = jax.random.normal(rng, shape, jnp.float32) * deviation * factor_of
    return jnp.minimum(jnp.maximum(drawn, -most), most).astype(held_as)


def gaussian_with(rng, dims, deviation, limit, shards, heavy, kind=jnp.bfloat16):
    result = deviation * jax.random.normal(rng, dims, jnp.float32)
    if shards:
        result = result * block_scale(rng, dims, shards, -0.22, 0.18)
    return jnp.clip(raised(result, jax.random.fold_in(rng, 3), *heavy), -limit, limit).astype(kind)


def setup_inputs(seed: int = 0) -> dict:
    streams_of = jax.random.split(jax.random.key(seed), 14)
    glu_a = normal_values(streams_of[0], (TOKENS, CONV_CHANNELS), 1.0, 6.0, ((0, 8), (1, 4)))
    glu_b = normal_values(streams_of[1], (TOKENS, CONV_CHANNELS), 1.0, 6.0, ((0, 8), (1, 4)))
    saved_conv = draw_saved_conv(jax.random.fold_in(streams_of[13], 71), 0)
    taps = normal_values(streams_of[3], (KW, CONV_CHANNELS), 0.18, 1.0, ((1, 4),), jnp.float32)
    norm_gain_vector = jnp.clip(1.0 + 0.18 * jax.random.normal(streams_of[4], (CONV_CHANNELS,), jnp.float32), 0.1, 1.9)
    out_proj = normal_values(streams_of[5], (CONV_CHANNELS, D), CONV_CHANNELS ** -0.5, 0.1875, ((0, 4),))
    moe_in = normal_values(streams_of[6], (TOKENS, D), 1.0, 6.0, ((0, 8),))
    grad_out = gaussian_with(streams_of[7], (TOKENS, D), 1.0, 6.0, ((0, 8),), (0, 1, 8, 2.0))
    expert_ids_keys = jax.random.split(jax.random.fold_in(streams_of[8], 1), TOKENS // TOK_DEV)
    expert_ids_turns = jax.random.permutation(jax.random.fold_in(streams_of[8], 3), TOKENS // TOK_DEV)
    expert_ids = jax.vmap(lambda own, number: deal_out(jax.random.fold_in(streams_of[8], 2), own, number, TOK_DEV, EXPERTS, TOPK, CAP, 1))(expert_ids_keys, expert_ids_turns).reshape((TOKENS, TOPK))
    route_weights = jnp.clip(0.3 + 1.7 * jax.random.uniform(streams_of[9], (TOKENS, TOPK), jnp.float32) ** block_scale(streams_of[9], (TOKENS, TOPK), ((0, 8),), -0.2, 0.2), 0.3, 2.0)
    w_gate = normal_values(streams_of[10], (EXPERTS, D, FF), D ** -0.5, 0.125, ((0, 8), (2, 4)))
    w_up = normal_values(streams_of[11], (EXPERTS, D, FF), D ** -0.5, 0.125, ((0, 8), (2, 4)))
    w_down = normal_values(streams_of[12], (EXPERTS, FF, D), FF ** -0.5, 0.1875, ((0, 8), (1, 4)))
    return {"glu_a": glu_a, "glu_b": glu_b, "saved_conv": saved_conv, "taps": taps, "norm_gain_vector": norm_gain_vector, "out_proj": out_proj, "moe_in": moe_in, "grad_out": grad_out, "expert_ids": expert_ids, "route_weights": route_weights, "w_gate": w_gate, "w_up": w_up, "w_down": w_down}


def expert_backward(item):
    in_rows, cot_rows, gate_w, up_w, down_w = item
    gate_pre = jnp.dot(in_rows, gate_w, preferred_element_type=jnp.float32)
    up_pre = jnp.dot(in_rows, up_w, preferred_element_type=jnp.float32)
    sig_gate = jax.nn.sigmoid(gate_pre)
    act_gate = gate_pre * sig_gate
    hidden = (act_gate * up_pre).astype(jnp.bfloat16)
    grad_hidden = jnp.dot(cot_rows, down_w.T, preferred_element_type=jnp.float32)
    grad_upact = (grad_hidden * act_gate).astype(jnp.bfloat16)
    grad_gateact = (grad_hidden * up_pre * sig_gate * (1.0 + gate_pre * (1.0 - sig_gate))).astype(jnp.bfloat16)
    grad_down = jnp.dot(hidden.T, cot_rows, preferred_element_type=jnp.float32).astype(jnp.bfloat16)
    grad_gate = jnp.dot(in_rows.T, grad_gateact, preferred_element_type=jnp.float32).astype(jnp.bfloat16)
    grad_up = jnp.dot(in_rows.T, grad_upact, preferred_element_type=jnp.float32).astype(jnp.bfloat16)
    rows_n = in_rows.shape[0]
    part_ff = FF // N_TP
    g_split = grad_gateact.astype(jnp.float32).reshape(rows_n, N_TP, part_ff)
    u_split = grad_upact.astype(jnp.float32).reshape(rows_n, N_TP, part_ff)
    wg_split = gate_w.astype(jnp.float32).reshape(D, N_TP, part_ff)
    wu_split = up_w.astype(jnp.float32).reshape(D, N_TP, part_ff)
    partial_value = jnp.einsum('sqf,dqf->qsd', g_split, wg_split) + jnp.einsum('sqf,dqf->qsd', u_split, wu_split)
    partial_value = partial_value.astype(jnp.bfloat16).astype(jnp.float32)
    row_grads = lax.optimization_barrier(jnp.sum(partial_value, axis=0)).astype(jnp.bfloat16)
    return (grad_gate, grad_up, grad_down, row_grads)

def reference(glu_a, glu_b, saved_conv, taps, norm_gain_vector, out_proj, moe_in, grad_out, expert_ids, route_weights, w_gate, w_up, w_down):
    per_expert = N_SP * CAP
    pairs = TOKENS * TOPK
    flat_ids = expert_ids.reshape(N_SP, TOK_DEV * TOPK)
    onehot = (flat_ids[:, :, None] == jnp.arange(EXPERTS, dtype=jnp.int32)[None, None, :]).astype(jnp.int32)
    slot_rank = lax.optimization_barrier(jnp.sum((jnp.cumsum(onehot, axis=1) - onehot) * onehot, axis=2))
    source = jnp.arange(N_SP, dtype=jnp.int32)[:, None]
    slots = (flat_ids * per_expert + source * CAP + slot_rank).reshape(pairs).astype(jnp.int32)
    owner_idx = jnp.full((EXPERTS * per_expert,), pairs, jnp.int32).at[slots].set(jnp.arange(pairs, dtype=jnp.int32))
    token_idx = owner_idx // TOPK
    in_pad = jnp.concatenate([moe_in, jnp.zeros((1, D), jnp.bfloat16)], axis=0)
    in_rows = in_pad[token_idx].reshape(EXPERTS, per_expert, D)
    scaled = (grad_out.astype(jnp.float32)[:, None, :] * route_weights[:, :, None]).astype(jnp.bfloat16)
    cot_pad = jnp.concatenate([scaled.reshape(pairs, D), jnp.zeros((1, D), jnp.bfloat16)], axis=0)
    cot_rows = cot_pad[owner_idx].reshape(EXPERTS, per_expert, D)
    grad_gate, grad_up, grad_down, row_grads = lax.map(expert_backward, (in_rows, cot_rows, w_gate, w_up, w_down))
    picked = row_grads.reshape(EXPERTS * per_expert, D)[slots].reshape(TOKENS, TOPK, D)
    grad_moe = lax.optimization_barrier(jnp.sum(picked.astype(jnp.float32), axis=1))
    grad_mix = (grad_out.astype(jnp.float32) + grad_moe).astype(jnp.bfloat16)
    head_gradient = jnp.dot(grad_mix, out_proj.T, preferred_element_type=jnp.float32)
    convolved_rows = saved_conv.astype(jnp.float32)
    channel_average = lax.optimization_barrier(jnp.mean(convolved_rows, axis=1, keepdims=True))
    var_c = lax.optimization_barrier(jnp.mean(convolved_rows * convolved_rows, axis=1, keepdims=True)) - channel_average * channel_average
    inverse_deviation = lax.rsqrt(var_c + 1e-05)
    centered_scaled = (convolved_rows - channel_average) * inverse_deviation
    normalized_rows = centered_scaled * norm_gain_vector[None, :]
    sigmoid_of_norm = jax.nn.sigmoid(normalized_rows)
    heads = (normalized_rows * sigmoid_of_norm).astype(jnp.bfloat16)
    grad_out_proj = jnp.dot(grad_mix.T, heads, preferred_element_type=jnp.float32)
    normalized_gradient = head_gradient * sigmoid_of_norm * (1.0 + normalized_rows * (1.0 - sigmoid_of_norm)) * norm_gain_vector[None, :]
    gradient_average = lax.optimization_barrier(jnp.mean(normalized_gradient, axis=1, keepdims=True))
    product_average = lax.optimization_barrier(jnp.mean(normalized_gradient * centered_scaled, axis=1, keepdims=True))
    convolved_gradient = (inverse_deviation * (normalized_gradient - gradient_average - centered_scaled * product_average)).astype(jnp.bfloat16)
    reach = (KW - 1) // 2
    padded = jnp.pad(convolved_gradient, ((reach, reach), (0, 0))).astype(jnp.float32)
    grad_y = jnp.zeros((TOKENS, CONV_CHANNELS), jnp.float32)
    for tap_idx in range(KW):
        grad_y = grad_y + taps[tap_idx][None, :] * padded[2 * reach - tap_idx:2 * reach - tap_idx + TOKENS]
    sig_b = jax.nn.sigmoid(glu_b.astype(jnp.float32))
    grad_glu_a = (grad_y * sig_b).astype(jnp.bfloat16)
    grad_glu_b = (grad_y * glu_a.astype(jnp.float32) * sig_b * (1.0 - sig_b)).astype(jnp.bfloat16)
    return (grad_glu_a, grad_glu_b, grad_out_proj, grad_gate, grad_up, grad_down)
```

```python
import functools
import jax
import jax.numpy as jnp
from jax import lax
from jax.experimental import pallas as pl
from jax.experimental.pallas import tpu as pltpu
from jax.sharding import PartitionSpec as P

MESH = pl.DeviceIdType.MESH
F32 = jnp.float32
BF16 = jnp.bfloat16
HALO = 16
VMEM_LIMIT = 60 * 1024 * 1024


def remote(src, dst, send_sem, recv_sem, device):
    return pltpu.make_async_remote_copy(
        src_ref=src, dst_ref=dst, send_sem=send_sem, recv_sem=recv_sem, device_id=device, device_id_type=MESH
    )


def place(n_sp, n_tp):
    s, t = lax.axis_index("sp"), lax.axis_index("tp")
    core = lax.rem(t, 2)
    mate = t + 1 - 2 * core
    across = lax.rem(t + 2, n_tp)
    return s, t, core, mate, across


def each_peer(s, n_sp, body):
    def step(off, carry):
        body(lax.rem(s + off, n_sp), lax.rem(s + n_sp - off, n_sp))
        return carry

    lax.fori_loop(1, n_sp, step, 0)


def each(n, body):
    def step(i, carry):
        body(i)
        return carry

    lax.fori_loop(0, n, step, 0)


def greet(s, t, n_sp, n_tp):
    barrier = pltpu.get_barrier_semaphore()

    def hello(to, _):
        pl.semaphore_signal(barrier, inc=1, device_id=(to, t), device_id_type=MESH)

    each_peer(s, n_sp, hello)
    for off in range(1, n_tp):
        pl.semaphore_signal(barrier, inc=1, device_id=(s, lax.rem(t + off, n_tp)), device_id_type=MESH)
    pl.semaphore_wait(barrier, n_sp + n_tp - 2)


def dispatch_kernel(n_sp, n_tp, in_ref, cot_ref, st_ref, in_out, cot_out, st_out,
                    i_s, i_r, if_s, if_r, c_s, c_r, cy_s, cy_r, cf_s, cf_r, cg_s, cg_r, st_s, st_r, loc):
    s, t, core, mate, across = place(n_sp, n_tp)
    half, quarter = in_ref.shape[2], cot_ref.shape[2]

    def ci(index):
        return pl.ds(pl.multiple_of(index * half, half), half)

    def cq(index):
        return pl.ds(pl.multiple_of(index * quarter, quarter), quarter)

    greet(s, t, n_sp, n_tp)

    def send_cot(p, dst):
        return remote(cot_ref.at[p], cot_out.at[dst, :, cq(t)], c_s.at[p], c_r.at[dst], (p, t))

    def send_in(p, dst):
        return remote(in_ref.at[p], in_out.at[dst, :, ci(core)], i_s.at[p], i_r.at[dst], (p, t))

    def start(to, _):
        send_cot(to, s).start()
        send_in(to, s).start()

    each_peer(s, n_sp, start)

    def stat(to, row):
        return remote(st_ref, st_out.at[row], st_s.at[to], st_r.at[row], (s, to))

    for off in range(1, n_tp):
        stat(lax.rem(t + off, n_tp), t).start()
    own = [
        pltpu.make_async_copy(in_ref.at[s], in_out.at[s, :, ci(core)], loc.at[0]),
        pltpu.make_async_copy(cot_ref.at[s], cot_out.at[s, :, cq(t)], loc.at[1]),
        pltpu.make_async_copy(st_ref, st_out.at[t], loc.at[2]),
    ]
    for copy in own:
        copy.start()

    def fwd_in(src, p, column):
        return remote(src, in_out.at[p, :, ci(column)], if_s.at[p], if_r.at[p], (s, mate))

    def over_y(src, p, column):
        return remote(src, cot_out.at[p, :, cq(column)], cy_s.at[p], cy_r.at[p], (s, across))

    def fwd_cot(src, p, column):
        return remote(src, cot_out.at[p, :, cq(column)], cf_s.at[p], cf_r.at[p], (s, mate))

    def fwd_far(src, p, column):
        return remote(src, cot_out.at[p, :, cq(column)], cg_s.at[p], cg_r.at[p], (s, mate))

    over_y(cot_ref.at[s], s, t).start()
    fwd_cot(cot_ref.at[s], s, t).start()
    fwd_in(in_ref.at[s], s, core).start()

    def far(p):
        over_y(cot_out.at[p, :, cq(across)], p, across).wait_recv()
        fwd_far(cot_out.at[p, :, cq(across)], p, across).start()

    def forward(_, p):
        send_cot(p, p).wait_recv()
        over_y(cot_out.at[p, :, cq(t)], p, t).start()
        fwd_cot(cot_out.at[p, :, cq(t)], p, t).start()
        send_in(p, p).wait_recv()
        fwd_in(in_out.at[p, :, ci(core)], p, core).start()

    each_peer(s, n_sp, forward)
    far(s)
    each_peer(s, n_sp, lambda _, p: far(p))
    for copy in own:
        copy.wait()
    mate_far = lax.rem(mate + 2, n_tp)

    def finish(p):
        fwd_cot(cot_out.at[p, :, cq(mate)], p, mate).wait_recv()
        fwd_far(cot_out.at[p, :, cq(mate_far)], p, mate_far).wait_recv()
        fwd_in(in_out.at[p, :, ci(1 - core)], p, 1 - core).wait_recv()
        over_y(cot_out.at[p, :, cq(t)], p, t).wait_send()
        fwd_cot(cot_out.at[p, :, cq(t)], p, t).wait_send()
        fwd_far(cot_out.at[p, :, cq(across)], p, across).wait_send()
        fwd_in(in_out.at[p, :, ci(core)], p, core).wait_send()

    each(n_sp, finish)

    def sent(to, _):
        send_cot(to, s).wait_send()
        send_in(to, s).wait_send()

    each_peer(s, n_sp, sent)
    for off in range(1, n_tp):
        other = lax.rem(t + off, n_tp)
        stat(other, other).wait_recv()
        stat(other, t).wait_send()


def dispatch(in_half, cot_quarter, stats, n_sp, n_tp):
    rows, half = in_half.shape[1:]
    vm = pl.BlockSpec(memory_space=pltpu.VMEM)
    per = [pltpu.SemaphoreType.DMA((n_sp,))] * 12
    return pl.pallas_call(
        functools.partial(dispatch_kernel, n_sp, n_tp),
        out_shape=(
            jax.ShapeDtypeStruct((n_sp, rows, 2 * half), BF16),
            jax.ShapeDtypeStruct((n_sp, rows, 2 * half), BF16),
            jax.ShapeDtypeStruct((n_tp,) + stats.shape, F32),
        ),
        in_specs=[vm] * 3,
        out_specs=(vm,) * 3,
        scratch_shapes=per
        + [pltpu.SemaphoreType.DMA((n_tp,)), pltpu.SemaphoreType.DMA((n_tp,)), pltpu.SemaphoreType.DMA((3,))],
        compiler_params=pltpu.CompilerParams(collective_id=0, has_side_effects=True, vmem_limit_bytes=VMEM_LIMIT),
        name="dispatch",
    )(in_half, cot_quarter, stats)


def return_kernel(n_sp, n_tp, chunks, part_ref, pick_ref, go_ref, mix_out, prt, sb, ret, tsend, trecv,
                  m_s, m_r, a_s, a_r, y_s, y_r, g_s, g_r):
    s, t, core, mate, across = place(n_sp, n_tp)
    rows, d_model = part_ref.shape[1:]
    half = d_model // 2
    width = half // chunks
    greet(s, t, n_sp, n_tp)

    def to_mate(p):
        columns = pl.ds(pl.multiple_of((1 - core) * half, half), half)
        return remote(part_ref.at[p, :, columns], prt.at[p], m_s.at[p], m_r.at[p], (s, mate))

    each_peer(s, n_sp, lambda p, _: to_mate(p).start())
    to_mate(s).start()

    def cols(index, k):
        return pl.ds(pl.multiple_of(index * half + k * width, width), width)

    def pair_sum(k, p):
        return (part_ref[p, :, cols(core, k)].astype(F32) + prt[p, :, k * width:(k + 1) * width].astype(F32)).astype(BF16)

    def back(k, p, dst):
        return remote(sb.at[k, p], ret.at[k, dst], a_s.at[k * n_sp + p], a_r.at[k * n_sp + dst], (p, t))

    def cross(k):
        return remote(tsend.at[k], trecv.at[k], y_s.at[k], y_r.at[k], (s, across))

    def share(k, index):
        return remote(mix_out.at[:, cols(index, k)], mix_out.at[:, cols(index, k)], g_s.at[k], g_r.at[k], (s, mate))

    for k in range(chunks):
        def post(p, _, k=k):
            if k == 0:
                to_mate(p).wait_recv()
            sb[k, p] = pair_sum(k, p)
            back(k, p, s).start()

        each_peer(s, n_sp, post)
        if k == 0:
            to_mate(s).wait_recv()
        ret[k, s] = pair_sum(k, s)

    def gather(k):
        each_peer(s, n_sp, lambda _, p: back(k, p, p).wait_recv())
        total = jnp.dot(pick_ref[...], ret[k].reshape(n_sp * rows, width), preferred_element_type=F32)
        tsend[k] = total.astype(BF16)
        cross(k).start()

    def mix(k):
        cross(k).wait_recv()
        mix_out[:, cols(core, k)] = (
            go_ref[:, cols(core, k)].astype(F32) + (tsend[k].astype(F32) + trecv[k].astype(F32))
        ).astype(BF16)
        share(k, core).start()

    for k in range(chunks):
        gather(k)
        if k:
            mix(k - 1)
    mix(chunks - 1)
    for k in range(chunks):
        share(k, 1 - core).wait_recv()
        share(k, core).wait_send()
        cross(k).wait_send()
        each_peer(s, n_sp, lambda p, _, k=k: back(k, p, s).wait_send())
    each(n_sp, lambda p: to_mate(p).wait_send())


def give_back(partial, pick, grad_out, n_sp, n_tp, chunks=2):
    rows, d_model = partial.shape[1:]
    tok = grad_out.shape[0]
    half = d_model // 2
    width = half // chunks
    vm = pl.BlockSpec(memory_space=pltpu.VMEM)
    dma = pltpu.SemaphoreType.DMA
    return pl.pallas_call(
        functools.partial(return_kernel, n_sp, n_tp, chunks),
        out_shape=jax.ShapeDtypeStruct((tok, d_model), BF16),
        in_specs=[vm] * 3,
        out_specs=vm,
        scratch_shapes=[
            pltpu.VMEM((n_sp, rows, half), BF16),
            pltpu.VMEM((chunks, n_sp, rows, width), BF16),
            pltpu.VMEM((chunks, n_sp, rows, width), BF16),
            pltpu.VMEM((chunks, tok, width), BF16),
            pltpu.VMEM((chunks, tok, width), BF16),
            dma((n_sp,)), dma((n_sp,)), dma((chunks * n_sp,)), dma((chunks * n_sp,)),
            dma((chunks,)), dma((chunks,)), dma((chunks,)), dma((chunks,)),
        ],
        compiler_params=pltpu.CompilerParams(collective_id=1, has_side_effects=True, vmem_limit_bytes=VMEM_LIMIT),
        name="give_back",
    )(partial, pick, grad_out)


def tail_kernel(n_sp, n_tp, mix_ref, proj_ref, conv_ref, st_ref, gain_ref, taps_ref, a_ref, b_ref,
                ga_out, gb_out, gop_out, sb, rb, cg, before, after, padded, st_in, st_all,
                p_s, p_r, q_s, q_r, h_s, h_r):
    s, t, core, mate, across = place(n_sp, n_tp)
    tok, width = conv_ref.shape
    share = mix_ref.shape[1] // n_sp
    channels = width * n_tp
    greet(s, t, n_sp, n_tp)
    conv = conv_ref[...].astype(F32)
    stats = st_ref[...]
    mean, rstd = stats[:, 0:1], stats[:, 1:2]
    xhat = (conv - mean) * rstd
    gain = gain_ref[...]
    normed = xhat * gain
    sig = jax.nn.sigmoid(normed)
    heads = (normed * sig).astype(BF16)
    piece = 512
    for i in range(mix_ref.shape[1] // piece):
        sb[i * piece:(i + 1) * piece, :] = lax.dot_general(
            mix_ref[:, i * piece:(i + 1) * piece], heads, (((0,), (0,)), ((), ())), preferred_element_type=F32
        ).astype(BF16)

    def rows_of(p):
        return pl.ds(pl.multiple_of(p * share, 16), share)

    def send(p, dst):
        return remote(sb.at[rows_of(p)], rb.at[dst], p_s.at[p], p_r.at[dst], (p, t))

    each_peer(s, n_sp, lambda p, _: send(p, s).start())

    head = lax.dot_general(mix_ref[...], proj_ref[...], (((1,), (1,)), ((), ())), preferred_element_type=F32)
    grad = head * sig * (1.0 + normed * (1.0 - sig)) * gain
    total = jnp.sum(grad, axis=1, keepdims=True)
    product = jnp.sum(grad * xhat, axis=1, keepdims=True)
    lane = lax.broadcasted_iota(jnp.int32, (tok, 128), 1)
    both = jnp.where(lane == 0, total, jnp.where(lane == 1, product, 0.0))
    st_in[...] = both.T[0:8, :]

    def stat(to, row):
        return remote(st_in, st_all.at[row], q_s.at[to], q_r.at[row], (s, to))

    for off in range(1, n_tp):
        stat(lax.rem(t + off, n_tp), t).start()
    st_all[t] = both.T[0:8, :]
    for off in range(1, n_tp):
        other = lax.rem(t + off, n_tp)
        stat(other, other).wait_recv()
    summed = st_all[0]
    for i in range(1, n_tp):
        summed = summed + st_all[i]
    wide = jnp.concatenate([summed, jnp.zeros((120, tok), F32)], axis=0).T
    cgrad = (
        rstd * (grad - wide[:, 0:1] / channels - xhat * (wide[:, 1:2] / channels))
    ).astype(BF16)
    cg[...] = cgrad

    up = remote(cg.at[tok - HALO:tok], before, h_s.at[0], h_r.at[0], (lax.rem(s + 1, n_sp), t))
    down = remote(cg.at[0:HALO], after, h_s.at[1], h_r.at[1], (lax.rem(s + n_sp - 1, n_sp), t))
    up.start()
    down.start()
    padded[HALO:HALO + tok, :] = cgrad.astype(F32)
    up.wait_recv()
    down.wait_recv()
    padded[0:HALO, :] = jnp.where(s > 0, before[...].astype(F32), 0.0)
    padded[HALO + tok:2 * HALO + tok, :] = jnp.where(s < n_sp - 1, after[...].astype(F32), 0.0)
    taps_n = taps_ref.shape[0]
    reach = (taps_n - 1) // 2
    block = 64
    for r in range(tok // block):
        acc = jnp.zeros((block, width), F32)
        for j in range(taps_n):
            first = r * block + HALO + reach - j
            acc = acc + taps_ref[j:j + 1, :] * padded[first:first + block, :]
        at = slice(r * block, (r + 1) * block)
        sig_b = jax.nn.sigmoid(b_ref[at, :].astype(F32))
        ga_out[at, :] = (acc * sig_b).astype(BF16)
        gb_out[at, :] = (acc * a_ref[at, :].astype(F32) * sig_b * (1.0 - sig_b)).astype(BF16)

    gop_out[...] = sb[rows_of(s), :].astype(F32)

    def add(_, p):
        send(p, p).wait_recv()
        gop_out[...] += rb[p].astype(F32)

    each_peer(s, n_sp, add)
    each_peer(s, n_sp, lambda p, _: send(p, s).wait_send())
    for off in range(1, n_tp):
        stat(lax.rem(t + off, n_tp), t).wait_send()
    up.wait_send()
    down.wait_send()


def tail(mix, proj, conv, stats, gain, taps, glu_a, glu_b, n_sp, n_tp):
    tok, width = conv.shape
    d_model = mix.shape[1]
    vm = pl.BlockSpec(memory_space=pltpu.VMEM)
    dma = pltpu.SemaphoreType.DMA
    return pl.pallas_call(
        functools.partial(tail_kernel, n_sp, n_tp),
        out_shape=(
            jax.ShapeDtypeStruct((tok, width), BF16),
            jax.ShapeDtypeStruct((tok, width), BF16),
            jax.ShapeDtypeStruct((d_model // n_sp, width), F32),
        ),
        in_specs=[vm] * 8,
        out_specs=(vm,) * 3,
        scratch_shapes=[
            pltpu.VMEM((d_model, width), BF16),
            pltpu.VMEM((n_sp, d_model // n_sp, width), BF16),
            pltpu.VMEM((tok, width), BF16),
            pltpu.VMEM((HALO, width), BF16),
            pltpu.VMEM((HALO, width), BF16),
            pltpu.VMEM((tok + 2 * HALO, width), F32),
            pltpu.VMEM((8, tok), F32),
            pltpu.VMEM((n_tp, 8, tok), F32),
            dma((n_sp,)), dma((n_sp,)), dma((n_tp,)), dma((n_tp,)), dma((2,)), dma((2,)),
        ],
        compiler_params=pltpu.CompilerParams(collective_id=2, has_side_effects=True, vmem_limit_bytes=VMEM_LIMIT),
        name="tail",
    )(mix, proj, conv, stats, gain, taps, glu_a, glu_b)


def expert_local(in_rows, cot_rows, w_gate, w_up, w_down):
    gate_pre = jnp.einsum("esd,edf->esf", in_rows, w_gate, preferred_element_type=jnp.float32)
    up_pre = jnp.einsum("esd,edf->esf", in_rows, w_up, preferred_element_type=jnp.float32)
    sig_gate = jax.nn.sigmoid(gate_pre)
    act_gate = gate_pre * sig_gate
    hidden = (act_gate * up_pre).astype(jnp.bfloat16)
    grad_hidden = jnp.einsum("esd,efd->esf", cot_rows, w_down, preferred_element_type=jnp.float32)
    grad_upact = (grad_hidden * act_gate).astype(jnp.bfloat16)
    grad_gateact = (grad_hidden * up_pre * sig_gate * (1.0 + gate_pre * (1.0 - sig_gate))).astype(
        jnp.bfloat16
    )
    return (hidden, grad_upact, grad_gateact)


def weight_grads(in_rows, cot_rows, hidden, grad_upact, grad_gateact):
    grad_down = jnp.einsum(
        "esf,esd->efd", hidden, cot_rows, preferred_element_type=jnp.float32
    ).astype(jnp.bfloat16)
    grad_gate = jnp.einsum(
        "esd,esf->edf", in_rows, grad_gateact, preferred_element_type=jnp.float32
    ).astype(jnp.bfloat16)
    grad_up = jnp.einsum(
        "esd,esf->edf", in_rows, grad_upact, preferred_element_type=jnp.float32
    ).astype(jnp.bfloat16)
    return (grad_gate, grad_up, grad_down)


def per_device(
    glu_a, glu_b, saved_conv, taps, norm_gain_vector, out_proj, moe_in, grad_out, expert_ids, route_weights,
    w_gate, w_up, w_down,
):
    n_sp = lax.axis_size("sp")
    n_tp = lax.axis_size("tp")
    tp_pos = lax.axis_index("tp")
    tok_dev, d_model = grad_out.shape
    top_count = expert_ids.shape[1]
    exp_dev = w_gate.shape[0]
    experts = exp_dev * n_sp
    capacity = max(2, 3 * tok_dev * top_count // (2 * experts))
    capacity = (capacity + 15) // 16 * 16
    channels = saved_conv.shape[1] * n_tp
    half, quarter = d_model // 2, d_model // n_tp
    chosen = expert_ids[:, :, None] == jnp.arange(experts, dtype=jnp.int32)[None, None, :]
    named = jnp.sum(chosen.astype(F32), axis=1)
    places = jnp.arange(tok_dev)
    earlier = (places[:, None] > places[None, :]).astype(BF16)
    before = jnp.dot(earlier, named.astype(BF16), preferred_element_type=F32)
    rank = jnp.sum(jnp.where(chosen, before[:, None, :], 0.0), axis=2).astype(jnp.int32)
    slot_of = expert_ids * capacity + rank
    slots = jnp.arange(experts * capacity, dtype=jnp.int32)
    hits = slot_of[:, :, None] == slots[None, None, :]
    pick = jnp.any(hits, axis=1).astype(BF16)
    row_weight = jnp.sum(jnp.where(hits, route_weights[:, :, None], 0.0), axis=(0, 1))
    in_part = lax.dynamic_slice_in_dim(moe_in, (tp_pos % 2) * half, half, 1)
    cot_part = lax.dynamic_slice_in_dim(grad_out, tp_pos * quarter, quarter, 1)

    def spread(part):
        return lax.dot_general(pick, part, (((0,), (0,)), ((), ())), preferred_element_type=F32)

    in_half = spread(in_part).astype(BF16).reshape(n_sp, exp_dev * capacity, half)
    cot_quarter = (spread(cot_part) * row_weight[:, None]).astype(BF16).reshape(n_sp, exp_dev * capacity, quarter)
    conv = saved_conv.astype(F32)
    sums = jnp.stack([jnp.sum(conv, axis=1), jnp.sum(conv * conv, axis=1)])
    sums = jnp.concatenate([sums, jnp.zeros((6, tok_dev), F32)])
    recv_in, recv_cot, all_sums = dispatch(in_half, cot_quarter, sums, n_sp, n_tp)

    def to_expert(rows):
        return (
            rows.reshape(n_sp, exp_dev, capacity, d_model).swapaxes(0, 1).reshape(exp_dev, n_sp * capacity, d_model)
        )

    in_rows = to_expert(recv_in)
    cot_rows = to_expert(recv_cot)
    hidden, grad_upact, grad_gateact = expert_local(in_rows, cot_rows, w_gate, w_up, w_down)
    partial_value = jnp.einsum("esf,edf->esd", grad_gateact, w_gate, preferred_element_type=F32)
    partial_value = partial_value + jnp.einsum("esf,edf->esd", grad_upact, w_up, preferred_element_type=F32)
    partial_value = (
        partial_value.astype(BF16)
        .reshape(exp_dev, n_sp, capacity, d_model)
        .swapaxes(0, 1)
        .reshape(n_sp, exp_dev * capacity, d_model)
    )
    grad_gate, grad_up, grad_down = weight_grads(in_rows, cot_rows, hidden, grad_upact, grad_gateact)
    grad_mix = give_back(partial_value, pick, grad_out, n_sp, n_tp)
    sum_c, sum_sq = jnp.sum(all_sums, axis=0)[0:2]
    mean = sum_c / channels
    rstd = lax.rsqrt(sum_sq / channels - mean * mean + 1e-05)
    stats = jnp.pad(jnp.stack([mean, rstd], axis=1), ((0, 0), (0, 126)))
    grad_glu_a, grad_glu_b, grad_out_proj = tail(
        grad_mix, out_proj, saved_conv, stats, norm_gain_vector[None, :], taps, glu_a, glu_b, n_sp, n_tp
    )
    return (grad_glu_a, grad_glu_b, grad_out_proj, grad_gate, grad_up, grad_down)


def solution(mesh):
    in_specs = (
        P("sp", "tp"),
        P("sp", "tp"),
        P("sp", "tp"),
        P(None, "tp"),
        P("tp"),
        P("tp", None),
        P("sp", None),
        P("sp", None),
        P("sp", None),
        P("sp", None),
        P("sp", None, "tp"),
        P("sp", None, "tp"),
        P("sp", "tp", None),
    )
    out_specs = (
        P("sp", "tp"),
        P("sp", "tp"),
        P("sp", "tp"),
        P("sp", None, "tp"),
        P("sp", None, "tp"),
        P("sp", "tp", None),
    )
    return jax.shard_map(
        per_device, mesh=mesh, in_specs=in_specs, out_specs=out_specs, check_vma=False
    )
```

```python
import functools
import jax
import jax.numpy as jnp
from jax import lax
from jax.experimental import pallas as pl
from jax.experimental.pallas import tpu as pltpu
from jax.sharding import PartitionSpec as P

MESH = pl.DeviceIdType.MESH
F32 = jnp.float32
BF16 = jnp.bfloat16
HALO = 16
VMEM_LIMIT = 60 * 1024 * 1024


def remote(src, dst, send_sem, recv_sem, device):
    return pltpu.make_async_remote_copy(
        src_ref=src, dst_ref=dst, send_sem=send_sem, recv_sem=recv_sem, device_id=device, device_id_type=MESH
    )


def place(n_sp, n_tp):
    s, t = lax.axis_index("sp"), lax.axis_index("tp")
    core = lax.rem(t, 2)
    mate = t + 1 - 2 * core
    across = lax.rem(t + 2, n_tp)
    return s, t, core, mate, across


def offset_of(i, n_sp):
    return 1 + lax.rem(i + n_sp // 2 - 1, n_sp - 1)


def each_peer(s, n_sp, body):
    def step(i, carry):
        off = offset_of(i, n_sp)
        body(lax.rem(s + off, n_sp), lax.rem(s + n_sp - off, n_sp))
        return carry

    lax.fori_loop(0, n_sp - 1, step, 0)


def each(n, body):
    def step(i, carry):
        body(i)
        return carry

    lax.fori_loop(0, n, step, 0)


def greet(s, t, n_sp, n_tp):
    barrier = pltpu.get_barrier_semaphore()

    def hello(to, _):
        pl.semaphore_signal(barrier, inc=1, device_id=(to, t), device_id_type=MESH)

    each_peer(s, n_sp, hello)
    for off in range(1, n_tp):
        pl.semaphore_signal(barrier, inc=1, device_id=(s, lax.rem(t + off, n_tp)), device_id_type=MESH)
    pl.semaphore_wait(barrier, n_sp + n_tp - 2)


def dispatch_kernel(n_sp, n_tp, window, rows_ref, st_ref, rows_out, st_out,
                    c_s, c_r, y_s, y_r, f_s, f_r, g_s, g_r, st_s, st_r, loc):
    s, t, core, mate, across = place(n_sp, n_tp)
    quarter = rows_ref.shape[3]
    peers = n_sp - 1
    mate_far = lax.rem(mate + 2, n_tp)

    def cq(index):
        return pl.ds(pl.multiple_of(index * quarter, quarter), quarter)

    def landed(m, p, index):
        return rows_out.at[m, p, :, cq(index)]

    greet(s, t, n_sp, n_tp)

    def send(m, p, dst):
        return remote(rows_ref.at[m, p], landed(m, dst, t), c_s.at[m * n_sp + p], c_r.at[m * n_sp + dst], (p, t))

    def over_y(src, m, p, index):
        return remote(src, landed(m, p, index), y_s.at[m * n_sp + p], y_r.at[m * n_sp + p], (s, across))

    def near(src, m, p, index):
        return remote(src, landed(m, p, index), f_s.at[m * n_sp + p], f_r.at[m * n_sp + p], (s, mate))

    def far(src, m, p, index):
        return remote(src, landed(m, p, index), g_s.at[m * n_sp + p], g_r.at[m * n_sp + p], (s, mate))

    def stat(to, row):
        return remote(st_ref, st_out.at[row], st_s.at[to], st_r.at[row], (s, to))

    def start(j):
        p = lax.rem(s + offset_of(lax.rem(j, peers), n_sp), n_sp)
        send(j // peers, p, s).start()

    each(window, start)
    for off in range(1, n_tp):
        stat(lax.rem(t + off, n_tp), t).start()
    own = [pltpu.make_async_copy(st_ref, st_out.at[t], loc.at[2])]
    for m in range(2):
        own.append(pltpu.make_async_copy(rows_ref.at[m, s], landed(m, s, t), loc.at[m]))
        over_y(rows_ref.at[m, s], m, s, t).start()
        near(rows_ref.at[m, s], m, s, t).start()
    for copy in own:
        copy.start()

    def relay(m, p):
        over_y(landed(m, p, across), m, p, across).wait_recv()
        far(landed(m, p, across), m, p, across).start()

    def forward(j):
        m = j // peers
        p = lax.rem(s + n_sp - offset_of(lax.rem(j, peers), n_sp), n_sp)
        send(m, p, p).wait_recv()
        over_y(landed(m, p, t), m, p, t).start()
        near(landed(m, p, t), m, p, t).start()

    def paced(j):
        start(j + window)
        forward(j)

    each(2 * peers - window, paced)

    def rest(j, carry):
        forward(j)
        return carry

    lax.fori_loop(2 * peers - window, 2 * peers, rest, 0)
    for m in range(2):
        relay(m, s)
    for m in range(2):
        each_peer(s, n_sp, lambda _, p, m=m: relay(m, p))
    for copy in own:
        copy.wait()

    def finish(j):
        m, p = j // n_sp, lax.rem(j, n_sp)
        near(landed(m, p, mate), m, p, mate).wait_recv()
        far(landed(m, p, mate_far), m, p, mate_far).wait_recv()
        over_y(landed(m, p, t), m, p, t).wait_send()
        near(landed(m, p, t), m, p, t).wait_send()
        far(landed(m, p, across), m, p, across).wait_send()

    each(2 * n_sp, finish)
    for m in range(2):
        each_peer(s, n_sp, lambda p, _, m=m: send(m, p, s).wait_send())
    for off in range(1, n_tp):
        other = lax.rem(t + off, n_tp)
        stat(other, other).wait_recv()
        stat(other, t).wait_send()


def dispatch(pair, stats, n_sp, n_tp):
    rows, quarter = pair.shape[2:]
    vm = pl.BlockSpec(memory_space=pltpu.VMEM)
    dma = pltpu.SemaphoreType.DMA
    return pl.pallas_call(
        functools.partial(dispatch_kernel, n_sp, n_tp, min(6, n_sp - 1)),
        out_shape=(
            jax.ShapeDtypeStruct((2, n_sp, rows, n_tp * quarter), BF16),
            jax.ShapeDtypeStruct((n_tp,) + stats.shape, F32),
        ),
        in_specs=[vm] * 2,
        out_specs=(vm,) * 2,
        scratch_shapes=[dma((2 * n_sp,))] * 8 + [dma((n_tp,)), dma((n_tp,)), dma((3,))],
        compiler_params=pltpu.CompilerParams(collective_id=0, has_side_effects=True, vmem_limit_bytes=VMEM_LIMIT),
        name="dispatch",
    )(pair, stats)


def return_kernel(n_sp, n_tp, chunks, window, part_ref, pick_ref, go_ref, mix_out, prt, pair, yr, sb, ret,
                  m_s, m_r, y_s, y_r, a_s, a_r, b_s, b_r, f_s, f_r, g_s, g_r):
    s, t, core, mate, across = place(n_sp, n_tp)
    rows, d_model = part_ref.shape[1:]
    quarter = d_model // n_tp
    width = quarter // chunks
    mate_far = lax.rem(mate + 2, n_tp)
    steps = chunks * n_sp
    greet(s, t, n_sp, n_tp)

    def cq(index, k=0, size=quarter):
        return pl.ds(pl.multiple_of(index * quarter + k * width, width), size)

    def to_mate(p, which, index):
        return remote(
            part_ref.at[p, :, cq(index)], prt.at[which, p], m_s.at[which * n_sp + p], m_r.at[which * n_sp + p], (s, mate)
        )

    def target(i):
        return lax.rem(s + lax.rem(n_sp // 2 + i, n_sp), n_sp)

    def hand(i):
        p = target(i)
        to_mate(p, 1, mate_far).start()
        to_mate(p, 0, mate).start()

    each(n_sp, hand)

    def over_y(k, p):
        return remote(pair.at[k, p], yr.at[k, p], y_s.at[k * n_sp + p], y_r.at[k * n_sp + p], (s, across))

    def back(k, p, dst):
        return remote(sb.at[k, p], ret.at[k, dst], a_s.at[k * n_sp + p], a_r.at[k * n_sp + dst], (p, t))

    def summed(k, p, which, index):
        offset = pl.ds(pl.multiple_of(k * width, width), width)
        return part_ref[p, :, cq(index, k, width)].astype(F32) + prt[which, p, :, offset].astype(F32)

    def post(j):
        k, p = j // n_sp, target(lax.rem(j, n_sp))

        @pl.when(k == 0)
        def _():
            to_mate(p, 1, mate_far).wait_recv()
            to_mate(p, 0, mate).wait_recv()

        pair[k, p] = summed(k, p, 1, across).astype(BF16)
        over_y(k, p).start()

    def settle(j):
        k, p = j // n_sp, target(lax.rem(j, n_sp))
        over_y(k, p).wait_recv()
        sb[k, p] = (summed(k, p, 0, t) + yr[k, p].astype(F32)).astype(BF16)

        @pl.when(p != s)
        def _():
            back(k, p, s).start()

        @pl.when(p == s)
        def _():
            ret[k, s] = sb[k, p]

    each(window, post)

    def paced(j):
        post(j + window)
        settle(j)

    each(steps - window, paced)

    def rest(j, carry):
        settle(j)
        return carry

    lax.fori_loop(steps - window, steps, rest, 0)

    def share(k, index, send_sem, recv_sem, to):
        return remote(
            mix_out.at[:, cq(index, k, width)], mix_out.at[:, cq(index, k, width)], send_sem.at[k], recv_sem.at[k], (s, to)
        )

    for k in range(chunks):
        each_peer(s, n_sp, lambda _, p, k=k: back(k, p, p).wait_recv())
        total = jnp.dot(pick_ref[...], ret[k].reshape(n_sp * rows, width), preferred_element_type=F32)
        mix_out[:, cq(t, k, width)] = (go_ref[:, cq(t, k, width)].astype(F32) + total).astype(BF16)
        share(k, t, b_s, b_r, across).start()
        share(k, t, f_s, f_r, mate).start()
    for k in range(chunks):
        share(k, across, b_s, b_r, across).wait_recv()
        share(k, across, g_s, g_r, mate).start()
    for k in range(chunks):
        share(k, mate, f_s, f_r, mate).wait_recv()
        share(k, mate_far, g_s, g_r, mate).wait_recv()
        share(k, t, b_s, b_r, across).wait_send()
        share(k, t, f_s, f_r, mate).wait_send()
        share(k, across, g_s, g_r, mate).wait_send()
        each_peer(s, n_sp, lambda p, _, k=k: back(k, p, s).wait_send())

    def drained(p):
        to_mate(p, 1, mate_far).wait_send()
        to_mate(p, 0, mate).wait_send()
        for k in range(chunks):
            over_y(k, p).wait_send()

    each(n_sp, drained)


def give_back(partial, pick, grad_out, n_sp, n_tp, chunks=2):
    rows, d_model = partial.shape[1:]
    tok = grad_out.shape[0]
    quarter = d_model // n_tp
    vm = pl.BlockSpec(memory_space=pltpu.VMEM)
    dma = pltpu.SemaphoreType.DMA
    piece = pltpu.VMEM((chunks, n_sp, rows, quarter // chunks), BF16)
    return pl.pallas_call(
        functools.partial(return_kernel, n_sp, n_tp, chunks, min(6, n_sp)),
        out_shape=jax.ShapeDtypeStruct((tok, d_model), BF16),
        in_specs=[vm] * 3,
        out_specs=vm,
        scratch_shapes=[pltpu.VMEM((2, n_sp, rows, quarter), BF16)]
        + [piece] * 4
        + [dma((2 * n_sp,))] * 2
        + [dma((chunks * n_sp,))] * 4
        + [dma((chunks,))] * 6,
        compiler_params=pltpu.CompilerParams(collective_id=1, has_side_effects=True, vmem_limit_bytes=VMEM_LIMIT),
        name="give_back",
    )(partial, pick, grad_out)


def tail_kernel(n_sp, n_tp, mix_ref, proj_ref, conv_ref, st_ref, gain_ref, taps_ref,
                gy_out, rb, sb, nb, sb2, cg, before, after, padded, st_in, st_all,
                n_s, n_r, p_s, p_r, q_s, q_r, h_s, h_r):
    s, t, core, mate, across = place(n_sp, n_tp)
    tok, width = conv_ref.shape
    share = mix_ref.shape[1] // n_sp
    channels = width * n_tp
    greet(s, t, n_sp, n_tp)
    conv = conv_ref[...].astype(F32)
    stats = st_ref[...]
    mean, rstd = stats[:, 0:1], stats[:, 1:2]
    xhat = (conv - mean) * rstd
    gain = gain_ref[...]
    normed = xhat * gain
    sig = jax.nn.sigmoid(normed)
    heads = (normed * sig).astype(BF16)
    piece = 512
    for i in range(mix_ref.shape[1] // piece):
        sb[i * piece:(i + 1) * piece, :] = lax.dot_general(
            mix_ref[:, i * piece:(i + 1) * piece], heads, (((0,), (0,)), ((), ())), preferred_element_type=F32
        ).astype(BF16)

    def rows_of(p):
        return pl.ds(pl.multiple_of(p * share, 16), share)

    groups = n_sp // 2
    side, group = lax.rem(s, 2), s // 2
    partner = s + 1 - 2 * side

    def pool(g, index):
        return remote(sb.at[rows_of(2 * g + index)], nb.at[g], n_s.at[g], n_r.at[g], (partner, t))

    def send(g, dst):
        return remote(sb2.at[g], rb.at[dst], p_s.at[g], p_r.at[dst], (2 * g + side, t))

    def target(i):
        return lax.rem(group + lax.rem(groups // 2 + i, groups), groups)

    each(groups, lambda i: pool(target(i), 1 - side).start())

    head = lax.dot_general(mix_ref[...], proj_ref[...], (((1,), (1,)), ((), ())), preferred_element_type=F32)
    grad = head * sig * (1.0 + normed * (1.0 - sig)) * gain
    total = jnp.sum(grad, axis=1, keepdims=True)
    product = jnp.sum(grad * xhat, axis=1, keepdims=True)
    lane = lax.broadcasted_iota(jnp.int32, (tok, 128), 1)
    both = jnp.where(lane == 0, total, jnp.where(lane == 1, product, 0.0))
    st_in[...] = both.T[0:8, :]

    def stat(to, row):
        return remote(st_in, st_all.at[row], q_s.at[to], q_r.at[row], (s, to))

    for off in range(1, n_tp):
        stat(lax.rem(t + off, n_tp), t).start()
    st_all[t] = both.T[0:8, :]
    for off in range(1, n_tp):
        other = lax.rem(t + off, n_tp)
        stat(other, other).wait_recv()
    summed = st_all[0]
    for i in range(1, n_tp):
        summed = summed + st_all[i]
    wide = jnp.concatenate([summed, jnp.zeros((120, tok), F32)], axis=0).T
    cgrad = (
        rstd * (grad - wide[:, 0:1] / channels - xhat * (wide[:, 1:2] / channels))
    ).astype(BF16)
    cg[...] = cgrad

    up = remote(cg.at[tok - HALO:tok], before, h_s.at[0], h_r.at[0], (lax.rem(s + 1, n_sp), t))
    down = remote(cg.at[0:HALO], after, h_s.at[1], h_r.at[1], (lax.rem(s + n_sp - 1, n_sp), t))
    up.start()
    down.start()
    padded[HALO:HALO + tok, :] = cgrad.astype(F32)
    def pooled(i):
        g = target(i)
        pool(g, side).wait_recv()
        sb2[g] = (sb[rows_of(2 * g + side), :].astype(F32) + nb[g].astype(F32)).astype(BF16)

        @pl.when(g != group)
        def _():
            send(g, group).start()

        @pl.when(g == group)
        def _():
            rb[group] = sb2[g]

    each(groups, pooled)
    up.wait_recv()
    down.wait_recv()
    padded[0:HALO, :] = jnp.where(s > 0, before[...].astype(F32), 0.0)
    padded[HALO + tok:2 * HALO + tok, :] = jnp.where(s < n_sp - 1, after[...].astype(F32), 0.0)
    taps_n = taps_ref.shape[0]
    reach = (taps_n - 1) // 2
    block = 64
    for r in range(tok // block):
        acc = jnp.zeros((block, width), F32)
        for j in range(taps_n):
            first = r * block + HALO + reach - j
            acc = acc + taps_ref[j:j + 1, :] * padded[first:first + block, :]
        at = slice(r * block, (r + 1) * block)
        gy_out[at, :] = acc

    def others(body):
        each(groups, lambda g: pl.when(g != group)(lambda: body(g)))

    others(lambda g: send(g, g).wait_recv())
    others(lambda g: send(g, group).wait_send())
    each(groups, lambda g: pool(g, 1 - side).wait_send())
    for off in range(1, n_tp):
        stat(lax.rem(t + off, n_tp), t).wait_send()
    up.wait_send()
    down.wait_send()


def tail(mix, proj, conv, stats, gain, taps, n_sp, n_tp):
    tok, width = conv.shape
    d_model = mix.shape[1]
    vm = pl.BlockSpec(memory_space=pltpu.VMEM)
    dma = pltpu.SemaphoreType.DMA
    return pl.pallas_call(
        functools.partial(tail_kernel, n_sp, n_tp),
        out_shape=(
            jax.ShapeDtypeStruct((tok, width), F32),
            jax.ShapeDtypeStruct((n_sp // 2, d_model // n_sp, width), BF16),
        ),
        in_specs=[vm] * 6,
        out_specs=(vm,) * 2,
        scratch_shapes=[
            pltpu.VMEM((d_model, width), BF16),
            pltpu.VMEM((n_sp // 2, d_model // n_sp, width), BF16),
            pltpu.VMEM((n_sp // 2, d_model // n_sp, width), BF16),
            pltpu.VMEM((tok, width), BF16),
            pltpu.VMEM((HALO, width), BF16),
            pltpu.VMEM((HALO, width), BF16),
            pltpu.VMEM((tok + 2 * HALO, width), F32),
            pltpu.VMEM((8, tok), F32),
            pltpu.VMEM((n_tp, 8, tok), F32),
            dma((n_sp // 2,)), dma((n_sp // 2,)), dma((n_sp // 2,)), dma((n_sp // 2,)),
            dma((n_tp,)), dma((n_tp,)), dma((2,)), dma((2,)),
        ],
        compiler_params=pltpu.CompilerParams(collective_id=2, has_side_effects=True, vmem_limit_bytes=VMEM_LIMIT),
        name="tail",
    )(mix, proj, conv, stats, gain, taps)


def expert_local(in_rows, cot_rows, w_gate, w_up, w_down):
    gate_pre = jnp.einsum("esd,edf->esf", in_rows, w_gate, preferred_element_type=jnp.float32)
    up_pre = jnp.einsum("esd,edf->esf", in_rows, w_up, preferred_element_type=jnp.float32)
    sig_gate = jax.nn.sigmoid(gate_pre)
    act_gate = gate_pre * sig_gate
    hidden = (act_gate * up_pre).astype(jnp.bfloat16)
    grad_hidden = jnp.einsum("esd,efd->esf", cot_rows, w_down, preferred_element_type=jnp.float32)
    grad_upact = (grad_hidden * act_gate).astype(jnp.bfloat16)
    grad_gateact = (grad_hidden * up_pre * sig_gate * (1.0 + gate_pre * (1.0 - sig_gate))).astype(
        jnp.bfloat16
    )
    return (hidden, grad_upact, grad_gateact)


def weight_grads(in_rows, cot_rows, hidden, grad_upact, grad_gateact):
    grad_down = jnp.einsum(
        "esf,esd->efd", hidden, cot_rows, preferred_element_type=jnp.float32
    ).astype(jnp.bfloat16)
    grad_gate = jnp.einsum(
        "esd,esf->edf", in_rows, grad_gateact, preferred_element_type=jnp.float32
    ).astype(jnp.bfloat16)
    grad_up = jnp.einsum(
        "esd,esf->edf", in_rows, grad_upact, preferred_element_type=jnp.float32
    ).astype(jnp.bfloat16)
    return (grad_gate, grad_up, grad_down)


def per_device(
    glu_a, glu_b, saved_conv, taps, norm_gain_vector, out_proj, moe_in, grad_out, expert_ids, route_weights,
    w_gate, w_up, w_down,
):
    n_sp = lax.axis_size("sp")
    n_tp = lax.axis_size("tp")
    tp_pos = lax.axis_index("tp")
    tok_dev, d_model = grad_out.shape
    top_count = expert_ids.shape[1]
    exp_dev = w_gate.shape[0]
    experts = exp_dev * n_sp
    capacity = max(2, 3 * tok_dev * top_count // (2 * experts))
    capacity = (capacity + 15) // 16 * 16
    channels = saved_conv.shape[1] * n_tp
    quarter = d_model // n_tp
    chosen = expert_ids[:, :, None] == jnp.arange(experts, dtype=jnp.int32)[None, None, :]
    named = jnp.sum(chosen.astype(F32), axis=1)
    places = jnp.arange(tok_dev)
    earlier = (places[:, None] > places[None, :]).astype(BF16)
    before = jnp.dot(earlier, named.astype(BF16), preferred_element_type=F32)
    rank = jnp.sum(jnp.where(chosen, before[:, None, :], 0.0), axis=2).astype(jnp.int32)
    slot_of = expert_ids * capacity + rank
    slots = jnp.arange(experts * capacity, dtype=jnp.int32)
    hits = slot_of[:, :, None] == slots[None, None, :]
    pick = jnp.any(hits, axis=1).astype(BF16)
    row_weight = jnp.sum(jnp.where(hits, route_weights[:, :, None], 0.0), axis=(0, 1))
    in_part = lax.dynamic_slice_in_dim(moe_in, tp_pos * quarter, quarter, 1)
    cot_part = lax.dynamic_slice_in_dim(grad_out, tp_pos * quarter, quarter, 1)

    def spread(part):
        return lax.dot_general(pick, part, (((0,), (0,)), ((), ())), preferred_element_type=F32)

    pair = jnp.stack([spread(in_part).astype(BF16), (spread(cot_part) * row_weight[:, None]).astype(BF16)])
    pair = pair.reshape(2, n_sp, exp_dev * capacity, quarter)
    conv = saved_conv.astype(F32)
    sums = jnp.stack([jnp.sum(conv, axis=1), jnp.sum(conv * conv, axis=1)])
    sums = jnp.concatenate([sums, jnp.zeros((6, tok_dev), F32)])
    received, all_sums = dispatch(pair, sums, n_sp, n_tp)

    def to_expert(rows):
        return (
            rows.reshape(n_sp, exp_dev, capacity, d_model).swapaxes(0, 1).reshape(exp_dev, n_sp * capacity, d_model)
        )

    in_rows = to_expert(received[0])
    cot_rows = to_expert(received[1])
    hidden, grad_upact, grad_gateact = expert_local(in_rows, cot_rows, w_gate, w_up, w_down)
    partial_value = jnp.einsum("esf,edf->esd", grad_gateact, w_gate, preferred_element_type=F32)
    partial_value = partial_value + jnp.einsum("esf,edf->esd", grad_upact, w_up, preferred_element_type=F32)
    partial_value = (
        partial_value.astype(BF16)
        .reshape(exp_dev, n_sp, capacity, d_model)
        .swapaxes(0, 1)
        .reshape(n_sp, exp_dev * capacity, d_model)
    )
    grad_gate, grad_up, grad_down = weight_grads(in_rows, cot_rows, hidden, grad_upact, grad_gateact)
    grad_mix = give_back(partial_value, pick, grad_out, n_sp, n_tp)
    sum_c, sum_sq = jnp.sum(all_sums, axis=0)[0:2]
    mean = sum_c / channels
    rstd = lax.rsqrt(sum_sq / channels - mean * mean + 1e-05)
    stats = jnp.pad(jnp.stack([mean, rstd], axis=1), ((0, 0), (0, 126)))
    grad_y, shares = tail(grad_mix, out_proj, saved_conv, stats, norm_gain_vector[None, :], taps, n_sp, n_tp)
    grad_out_proj = jnp.sum(shares.astype(F32), axis=0)
    sig_b = jax.nn.sigmoid(glu_b.astype(F32))
    grad_glu_a = (grad_y * sig_b).astype(BF16)
    grad_glu_b = (grad_y * glu_a.astype(F32) * sig_b * (1.0 - sig_b)).astype(BF16)
    return (grad_glu_a, grad_glu_b, grad_out_proj, grad_gate, grad_up, grad_down)


def solution(mesh):
    in_specs = (
        P("sp", "tp"),
        P("sp", "tp"),
        P("sp", "tp"),
        P(None, "tp"),
        P("tp"),
        P("tp", None),
        P("sp", None),
        P("sp", None),
        P("sp", None),
        P("sp", None),
        P("sp", None, "tp"),
        P("sp", None, "tp"),
        P("sp", "tp", None),
    )
    out_specs = (
        P("sp", "tp"),
        P("sp", "tp"),
        P("sp", "tp"),
        P("sp", None, "tp"),
        P("sp", None, "tp"),
        P("sp", "tp", None),
    )
    return jax.shard_map(
        per_device, mesh=mesh, in_specs=in_specs, out_specs=out_specs, check_vma=False
    )
```
